32 devices in a mesh: grp: 2 (over y), sp: 4 (over z), tp: 4 (over x, core).
Axes of the slice: x: 2, y: 2, z: 4, core: 2. Of those that a mesh axis runs over, the one named last changes fastest.
Arguments:
- receptance: bfloat16 [1024, 1024], P(('grp', 'sp'), 'tp'), parts along dimension 0, may hold values from -6 to 6
- head_keys: bfloat16 [1024, 1024], P(('grp', 'sp'), 'tp'), parts along dimension 0, may hold values from -6 to 6
- head_values: bfloat16 [1024, 1024], P(('grp', 'sp'), 'tp'), parts along dimension 0, may hold values from -6 to 6
- decay_logits: bfloat16 [1024, 1024], P(('grp', 'sp'), 'tp'), parts along dimension 0, may hold values from -13 to 0
- decay_boost: float32 [1024, 1024], P(('grp', 'sp'), 'tp'), parts along dimension 0, may hold values from -1.4 to 0
- correction_logits: bfloat16 [1024, 1024], P(('grp', 'sp'), 'tp'), parts along dimension 0, may hold values from -6 to 4
- gate_logits: bfloat16 [1024, 1024], P(('grp', 'sp'), 'tp'), parts along dimension 0, may hold values from -8 to 8
- head_norm_gain: float32 [1024], P('tp'), may hold values from 0.1 to 1.9
- output_weight: bfloat16 [1024, 2048], P('tp'), may hold values from -0.1875 to 0.1875
- residual: bfloat16 [1024, 2048], P(('grp', 'sp', 'tp')), parts along dimension 0, may hold values from -4 to 4
- expert_norm_gain: float32 [2048], replicated, may hold values from 0.1 to 1.9
- routes: int32 [1024, 2], P(('grp', 'sp', 'tp')), parts along dimension 0, may hold values from 0 to 3, all different within a row; in each aligned block of 32 rows (0 to 31, 32 to 63, ...) at most 32 rows name the same one
- routing_weight: float32 [1024, 2], P(('grp', 'sp', 'tp')), parts along dimension 0, may hold values from 0.1 to 1
- expert_gate_weight: bfloat16 [4, 2048, 3584], P('sp', None, 'tp'), may hold values from -0.125 to 0.125
- expert_up_weight: bfloat16 [4, 2048, 3584], P('sp', None, 'tp'), may hold values from -0.125 to 0.125
- expert_down_weight: bfloat16 [4, 3584, 2048], P('sp', 'tp'), may hold values from -0.09375 to 0.09375
Outputs:
- layer_out: bfloat16 [1024, 2048], P(('grp', 'sp', 'tp')), parts along dimension 0
The draws below stay inside these ranges and needn't reach their ends.
There are 2 independent parts, one for each index of `grp`. The reference program is written for one: setup_inputs(seed, part) draws one part's arguments, and reference() takes and returns one part's arrays. A program takes and returns all parts, laid end to end along the dimension named above; an argument that names none is the same for every part. Nothing has to cross between parts.
Inputs may be any that keep to these rules, and one draw needn't show every extreme that they name: Each row names 2 different experts. Among the positions that one index of sp+tp holds in routes, no expert is named by more than 32 of them, and in every draw some expert is named by exactly 32 of them there.
All inputs are finite; a program needn't handle non-finite values.
Results may differ from the reference program's by a relative error of at most 0.017.
Values may be sent and summed in bfloat16 or wider, within the bound.
A program may use at most 64 MiB of HBM per device.

```python
import math
import jax
import jax.numpy as jnp
import numpy as np
from jax import lax

D = 2048
HEADS = 16
HEAD = 64
FF = 3584
TOP = 2
TOK_DEV = 128
TOKENS = 512
HW = 1024
HEADS_DEV = 4
FF_DEV = 896
EXPERTS = 4
CAP = 32
N_SP = 4
N_TP = 4


def head_speed(key):
    order = jax.random.permutation(jax.random.fold_in(key, 101), HEADS)
    return order < HEADS // 2


def draw_decay_logits(key, part):
    quick = head_speed(key)
    fast_level = jax.random.uniform(jax.random.fold_in(key, 1), (HEADS,), jnp.float32, -3.8, -2.6)
    slow_level = jax.random.uniform(jax.random.fold_in(key, 2), (HEADS,), jnp.float32, -10.0, -8.5)
    offset = jnp.where(quick, fast_level, slow_level)
    stretch = jax.random.uniform(jax.random.fold_in(key, 3), (TOKENS // TOK_DEV, HEADS), jnp.float32, -0.7, 0.7)
    stretch = jnp.repeat(stretch, TOK_DEV, axis=0)
    jitter = jnp.clip(0.6 * jax.random.normal(jax.random.fold_in(key, 4), (TOKENS, HEADS, HEAD), jnp.float32), -1.8, 1.8)
    values = offset[None, :, None] + stretch[:, :, None] + jitter
    return values.reshape(TOKENS, HEADS * HEAD).astype(jnp.bfloat16)


def draw_correction_logits(key, part):
    quick = head_speed(key)
    fast_level = jax.random.uniform(jax.random.fold_in(key, 11), (HEADS,), jnp.float32, -1.0, 1.0)
    slow_level = jax.random.uniform(jax.random.fold_in(key, 12), (HEADS,), jnp.float32, -3.0, -2.0)
    offset = jnp.where(quick, fast_level, slow_level)
    jitter = jnp.clip(0.7 * jax.random.normal(jax.random.fold_in(key, 13), (TOKENS, HEADS, HEAD), jnp.float32), -2.1, 2.1)
    values = offset[None, :, None] + jitter
    return values.reshape(TOKENS, HEADS * HEAD).astype(jnp.bfloat16)


def draw_decay_boost(key, part):
    places = jax.random.randint(jax.random.fold_in(key, 21), (2, HEADS), 0, TOKENS)
    depth = jnp.log(jax.random.uniform(jax.random.fold_in(key, 22), (2, HEADS, HEAD), jnp.float32, 0.5, 0.8))
    position = jnp.arange(TOKENS)[:, None]
    total = jnp.zeros((TOKENS, HEADS, HEAD), jnp.float32)
    for turn in range(2):
        struck = (position == places[turn][None, :]).astype(jnp.float32)
        total = total + struck[:, :, None] * depth[turn][None, :, :]
    return total.reshape(TOKENS, HEADS * HEAD)


def block_scale(stream_key, dims, cuts, least, largest):
    level, own = 1.0, jax.random.fold_in(stream_key, 6)
    for dim, parts in cuts:
        heights = jnp.exp(jax.random.uniform(jax.random.fold_in(own, dim), (parts,), jnp.float32, least / len(cuts), largest / len(cuts)))
        level = level * jnp.repeat(heights, dims[dim] // parts).reshape([-1 if axis == dim else 1 for axis in range(len(dims))])
    return level


def assign_block(key, own, number, rows, amount, top, limit, skew):
    ranking = jax.random.permutation(key, amount)
    packed, ordinary = load_shares(amount, rows * top, limit, skew, True), load_shares(amount, rows * top, limit, skew, False)
    places = jnp.arange(amount)

    def named(tallies, turn):
        used = int((tallies > 0).sum())
        fixed = max(1, used // 4)
        moved = fixed + (places - fixed + turn * (used - fixed)) % max(1, amount - fixed)
        return jnp.zeros((amount,), jnp.int32).at[ranking[jnp.where(places < fixed, places, moved)]].set(jnp.asarray(tallies, jnp.int32))

    tallies = jnp.where(number % 4 == 0, named(packed, number // 4), named(ordinary, number - number // 4 - 1))
    mixed = jax.random.permutation(jax.random.fold_in(own, 3), amount)
    donor, taker = mixed[0:amount // 2 * 2:2], mixed[1:amount // 2 * 2:2]
    room = jnp.minimum(tallies[donor] - 1, limit - tallies[taker]) // 2
    room = jnp.where((donor == ranking[0]) | (taker == ranking[0]) | (tallies[taker] == 0), 0, jnp.maximum(room, 0))
    moved = jax.random.randint(jax.random.fold_in(own, 4), (amount // 2,), 0, 1 << 20) % (room + 1)
    tallies = tallies.at[donor].add(-moved).at[taker].add(moved)
    items = jnp.searchsorted(jnp.cumsum(tallies), jnp.arange(rows * top), side="right").astype(jnp.int32)
    table = items.reshape(top, rows).T
    table = table[jax.random.permutation(jax.random.fold_in(own, 1), rows)]
    turn = jax.random.randint(jax.random.fold_in(own, 2), (rows, 1), 0, top)
    return jnp.take_along_axis(table, (jnp.arange(top)[None, :] + turn) % top, axis=1)


def load_shares(amount, total, limit, slope, full):
    loads = [(1 << 20) // math.isqrt(grade ** slope) + 1 for grade in range(1, amount + 1)]
    largest = limit if full else min(limit, max(-(-total // amount), total * loads[0] // sum(loads)))
    least = 1 if total - largest >= amount - 1 else 0
    given, rest = [largest] + [least] * (amount - 1), total - largest - least * (amount - 1)
    while rest > 0:
        free = [i for i in range(1, amount) if given[i] < largest] or [i for i in range(1, amount) if given[i] < limit]
        mass, left = sum([loads[i] for i in free]), rest
        for i in free:
            extra = min(limit - given[i], max(1, left * loads[i] // mass), rest)
            given[i] = given[i] + extra
            rest = rest - extra
    return np.array(given)


def normal_values(own_key, shape, scale, limit, pieces=(), kind=jnp.bfloat16):
    loudness = block_scale(own_key, shape, pieces, -0.22, 0.18) if pieces else 1.0
    values = jax.random.normal(own_key, shape, jnp.float32) * scale * loudness
    return jnp.minimum(jnp.maximum(values, -limit), limit).astype(kind)


def setup_inputs(seed: int = 0, part: int = 0) -> dict:
    arg_keys = jax.random.split(jax.random.key(seed), 17)
    part_keys = jax.random.split(jax.random.fold_in(arg_keys[16], part), 17)
    receptance = normal_values(part_keys[0], (TOKENS, HW), 1.0, 6.0, ((0, 4), (1, 4)))
    head_keys = normal_values(part_keys[1], (TOKENS, HW), 1.0, 6.0, ((0, 4), (1, 4)))
    head_values = normal_values(part_keys[2], (TOKENS, HW), 1.0, 6.0, ((0, 4), (1, 4)))
    decay_logits = draw_decay_logits(jax.random.fold_in(jax.random.fold_in(arg_keys[16], part), 71), part)
    decay_boost = draw_decay_boost(jax.random.fold_in(jax.random.fold_in(arg_keys[16], part), 71), part)
    correction_logits = draw_correction_logits(jax.random.fold_in(jax.random.fold_in(arg_keys[16], part), 71), part)
    gate_logits = normal_values(part_keys[6], (TOKENS, HW), 1.5, 8.0, ((0, 4), (1, 4)))
    head_norm_gain = jnp.clip(1.0 + 0.18 * jax.random.normal(arg_keys[7], (HW,), jnp.float32), 0.1, 1.9)
    output_weight = normal_values(arg_keys[8], (HW, D), HW ** -0.5, 0.1875, ((0, 4),))
    residual = normal_values(part_keys[9], (TOKENS, D), 0.5, 4.0, ((0, 16),))
    expert_norm_gain = jnp.clip(1.0 + 0.18 * jax.random.normal(arg_keys[10], (D,), jnp.float32), 0.1, 1.9)
    routes_keys = jax.random.split(jax.random.fold_in(part_keys[11], 1), TOKENS // (TOK_DEV // N_TP))
    routes_turns = jax.random.permutation(jax.random.fold_in(part_keys[11], 3), TOKENS // (TOK_DEV // N_TP))
    routes = jax.vmap(lambda own, number: assign_block(jax.random.fold_in(part_keys[11], 2), own, number, TOK_DEV // N_TP, EXPERTS, TOP, CAP, 2))(routes_keys, routes_turns).reshape((TOKENS, TOP))
    routing_weight = jnp.clip(0.1 + 0.9 * jax.random.uniform(part_keys[12], (TOKENS, TOP), jnp.float32) ** block_scale(part_keys[12], (TOKENS, TOP), ((0, 16),), -0.2, 0.2), 0.1, 1.0)
    expert_gate_weight = normal_values(arg_keys[13], (EXPERTS, D, FF), D ** -0.5, 0.125, ((0, 4), (2, 4)))
    expert_up_weight = normal_values(arg_keys[14], (EXPERTS, D, FF), D ** -0.5, 0.125, ((0, 4), (2, 4)))
    expert_down_weight = normal_values(arg_keys[15], (EXPERTS, FF, D), FF ** -0.5, 0.09375, ((0, 4), (1, 4)))
    return {"receptance": receptance, "head_keys": head_keys, "head_values": head_values, "decay_logits": decay_logits, "decay_boost": decay_boost, "correction_logits": correction_logits, "gate_logits": gate_logits, "head_norm_gain": head_norm_gain, "output_weight": output_weight, "residual": residual, "expert_norm_gain": expert_norm_gain, "routes": routes, "routing_weight": routing_weight, "expert_gate_weight": expert_gate_weight, "expert_up_weight": expert_up_weight, "expert_down_weight": expert_down_weight}


highest = lax.Precision.HIGHEST

def heads_divide(array):
    return array.astype(jnp.float32).reshape(array.shape[0], HEADS, HEAD)

def recurrence(state, inputs):
    query, decay_factor, keyed, valued, remove, insert = inputs
    along = jnp.einsum('hvk,hk->hv', state, remove, precision=highest)
    state = state * decay_factor[:, None, :] + along[:, :, None] * insert[:, None, :] + valued[:, :, None] * keyed[:, None, :]
    return (state, jnp.einsum('hvk,hk->hv', state, query, precision=highest))

def reference(receptance, head_keys, head_values, decay_logits, decay_boost, correction_logits, gate_logits, head_norm_gain, output_weight, residual, expert_norm_gain, routes, routing_weight, expert_gate_weight, expert_up_weight, expert_down_weight):
    query = heads_divide(receptance)
    keyed = heads_divide(head_keys)
    valued = heads_divide(head_values)
    unit = keyed * lax.rsqrt(lax.optimization_barrier(jnp.sum(keyed * keyed, axis=-1, keepdims=True)) + 1e-06)
    rate = jax.nn.sigmoid(heads_divide(correction_logits))
    decay_factor = jnp.exp(-jnp.exp(-jax.nn.softplus(-heads_divide(decay_logits)) - 0.5) + heads_divide(decay_boost))
    start = jnp.zeros((HEADS, HEAD, HEAD), jnp.float32)
    _, mixed = lax.scan(recurrence, start, (query, decay_factor, keyed, valued, -unit, unit * rate))
    centre = mixed - lax.optimization_barrier(jnp.mean(mixed, axis=-1, keepdims=True))
    spread = lax.optimization_barrier(jnp.mean(centre * centre, axis=-1, keepdims=True))
    normed = centre * lax.rsqrt(spread + 0.00064) * head_norm_gain.reshape(HEADS, HEAD)
    gated = (normed.reshape(TOKENS, HW) * jax.nn.sigmoid(gate_logits.astype(jnp.float32))).astype(jnp.bfloat16)
    group = HEADS_DEV * HEAD
    branch = jnp.zeros((TOKENS, D), jnp.float32)
    for group_index in range(N_TP):
        lower = group_index * group
        piece = jnp.dot(gated[:, lower:lower + group], output_weight[lower:lower + group], preferred_element_type=jnp.float32).astype(jnp.bfloat16)
        piece = lax.optimization_barrier(piece)
        branch = branch + piece.astype(jnp.float32)
    stream = residual.astype(jnp.float32) + branch
    normal = (stream * lax.rsqrt(lax.optimization_barrier(jnp.mean(stream * stream, axis=-1, keepdims=True)) + 1e-06) * expert_norm_gain).astype(jnp.bfloat16)
    flat_routes = routes.reshape(-1).astype(jnp.int32)
    most_rows = CAP * N_SP * N_TP

    def per_expert(total, item):
        gate_w, up_w, down_w, expert_index = item
        chosen = flat_routes == expert_index
        order = jnp.argsort(jnp.where(chosen, 0, 1).astype(jnp.int32), stable=True)[:most_rows].astype(jnp.int32)
        live = chosen[order]
        rows = normal[order // TOP]
        hidden = (jax.nn.silu(jnp.dot(rows, gate_w, preferred_element_type=jnp.float32)) * jnp.dot(rows, up_w, preferred_element_type=jnp.float32)).astype(jnp.bfloat16)
        result = jnp.zeros((most_rows, D), jnp.float32)
        for slice_index in range(N_TP):
            lower = slice_index * FF_DEV
            piece = jnp.dot(hidden[:, lower:lower + FF_DEV], down_w[lower:lower + FF_DEV], preferred_element_type=jnp.float32).astype(jnp.bfloat16)
            piece = lax.optimization_barrier(piece)
            result = result + piece.astype(jnp.float32)
        result = lax.optimization_barrier(result.astype(jnp.bfloat16)).astype(jnp.float32)
        total = total.at[order].add(jnp.where(live[:, None], result, jnp.float32(0.0)))
        return (total, None)
    pairs, _ = lax.scan(per_expert, jnp.zeros((TOKENS * TOP, D), jnp.float32), (expert_gate_weight, expert_up_weight, expert_down_weight, jnp.arange(EXPERTS, dtype=jnp.int32)))
    routed = lax.optimization_barrier(jnp.sum(pairs.reshape(TOKENS, TOP, D) * routing_weight[:, :, None], axis=1))
    return (stream + routed).astype(jnp.bfloat16)
```

```python
from functools import partial

import jax
import jax.numpy as jnp
from jax import lax
from jax.experimental import pallas as pl
from jax.experimental.pallas import tpu as pltpu
from jax.sharding import PartitionSpec as P

HEAD = 64
TOP = 2
BLK = 32
TOK_DEV = 128


highest = lax.Precision.HIGHEST


MESH = pl.DeviceIdType.MESH


def share_kernel(size, own_ref, all_ref, send_sem, recv_sem):
    me = lax.axis_index("sp")
    barrier = pltpu.get_barrier_semaphore()
    for k in range(1, size):
        peer = lax.rem(me + k, size)
        pl.semaphore_signal(barrier, inc=1, device_id={"sp": peer}, device_id_type=MESH)
    pl.semaphore_wait(barrier, size - 1)

    def transfer(slot, peer):
        return pltpu.make_async_remote_copy(
            src_ref=own_ref,
            dst_ref=all_ref.at[slot],
            send_sem=send_sem.at[peer],
            recv_sem=recv_sem.at[slot],
            device_id={"sp": peer},
            device_id_type=MESH,
        )

    def each(action):
        def step(peer, carry):
            action(peer)
            return carry

        lax.fori_loop(0, size, step, 0)

    def send(peer):
        @pl.when(peer > me)
        def _():
            transfer(me, peer).start()

        @pl.when(peer >= me)
        def _():
            all_ref[peer] = jnp.zeros(own_ref.shape, own_ref.dtype)

    def finish(peer):
        @pl.when(peer > me)
        def _():
            transfer(me, peer).wait_send()

        @pl.when(peer < me)
        def _():
            transfer(peer, peer).wait_recv()

    each(send)
    each(finish)


def prefix(x, axis, combine, identity):
    size, index = (lax.axis_size(axis), lax.axis_index(axis))
    own = jnp.concatenate([part.astype(jnp.bfloat16) for part in x], axis=-1)
    everything = pl.pallas_call(
        partial(share_kernel, size),
        out_shape=jax.ShapeDtypeStruct((size,) + own.shape, own.dtype),
        in_specs=[pl.BlockSpec(memory_space=pltpu.VMEM)],
        out_specs=pl.BlockSpec(memory_space=pltpu.VMEM),
        scratch_shapes=[pltpu.SemaphoreType.DMA((size,)), pltpu.SemaphoreType.DMA((size,))],
        compiler_params=pltpu.CompilerParams(collective_id=1, has_side_effects=True),
    )(own)
    before = identity
    for k in range(size):
        item = (
            everything[k, :, :, :HEAD].astype(jnp.float32),
            everything[k, :, :, HEAD:].astype(jnp.float32),
        )
        new = combine(before, item)
        before = jax.tree.map(lambda p, q: jnp.where(k < index, p, q), new, before)
    return before


def tail_kernel(
    sp_count,
    tp_count,
    cap,
    gated_ref,
    out_weight_ref,
    residual_ref,
    gain_ref,
    place_ref,
    combine_ref,
    gate_hbm,
    up_hbm,
    down_hbm,
    result_ref,
    gate_ref,
    up_ref,
    down_ref,
    part,
    part_in,
    stream_ref,
    outbound,
    rows,
    partial_ref,
    pair_in,
    cross_out,
    cross_in,
    final_ref,
    returned,
    weight_sem,
    part_send,
    part_recv,
    out_send,
    out_recv,
    fan_send,
    row_recv,
    pair_send,
    pair_recv,
    cross_send,
    cross_recv,
    final_send,
    final_recv,
):
    sp, tp = lax.axis_index("sp"), lax.axis_index("tp")
    chips = tp_count // 2
    chip, core = tp // 2, lax.rem(tp, 2)
    partner = chip * 2 + 1 - core
    local = residual_ref.shape[0]
    f32, bf16 = jnp.float32, jnp.bfloat16

    weights = [
        pltpu.make_async_copy(source.at[0], target, weight_sem.at[n])
        for n, (source, target) in enumerate(
            ((gate_hbm, gate_ref), (up_hbm, up_ref), (down_hbm, down_ref))
        )
    ]
    for copy in weights:
        copy.start()

    barrier = pltpu.get_barrier_semaphore()
    for k in range(1, sp_count):
        peer = lax.rem(sp + k, sp_count)
        pl.semaphore_signal(barrier, inc=1, device_id={"sp": peer}, device_id_type=MESH)
    for k in range(1, tp_count):
        peer = lax.rem(tp + k, tp_count)
        pl.semaphore_signal(barrier, inc=1, device_id={"tp": peer}, device_id_type=MESH)
    pl.semaphore_wait(barrier, sp_count + tp_count - 2)

    def remote(source, target, send, recv, where):
        return pltpu.make_async_remote_copy(
            src_ref=source,
            dst_ref=target,
            send_sem=send,
            recv_sem=recv,
            device_id=where,
            device_id_type=MESH,
        )

    def loop(count, action):
        def step(k, carry):
            action(k)
            return carry

        lax.fori_loop(0, count, step, 0)

    def part_copy(slot, peer):
        return remote(
            part.at[peer], part_in.at[slot], part_send.at[peer], part_recv.at[slot], {"tp": peer}
        )

    for k in range(1, tp_count + 1):
        peer = lax.rem(tp + k, tp_count)
        piece = gated_ref[pl.ds(pl.multiple_of(peer * local, local), local), :]
        part[peer] = jnp.dot(piece, out_weight_ref[...], preferred_element_type=f32).astype(bf16)
        if k < tp_count:
            part_copy(tp, peer).start()
    stream = residual_ref[...].astype(f32) + part[tp].astype(f32)
    for k in range(1, tp_count):
        peer = lax.rem(tp + tp_count - k, tp_count)
        part_copy(peer, peer).wait_recv()
        stream = stream + part_in[peer].astype(f32)
    stream_ref[...] = stream
    normal = (
        stream
        * lax.rsqrt(jnp.mean(stream * stream, axis=-1, keepdims=True) + 1e-06)
        * gain_ref[...]
    ).astype(bf16)
    sent = jnp.dot(place_ref[...], normal, preferred_element_type=f32).astype(bf16)
    outbound[...] = sent.reshape(outbound.shape)

    def block(ref, s, t):
        return ref.at[s, pl.ds(pl.multiple_of(t * cap, cap), cap)]

    def out_copy(slot, peer):
        return remote(
            outbound.at[peer],
            block(rows, slot, tp),
            out_send.at[peer],
            out_recv.at[slot],
            {"sp": peer},
        )

    def own_block(s):
        return block(rows, s, tp)

    def fan_copy(s, t, peer, slot):
        return remote(
            block(rows, s, t),
            block(rows, s, t),
            fan_send.at[s, slot],
            row_recv.at[s, t],
            {"tp": peer},
        )

    rows[sp, pl.ds(pl.multiple_of(tp * cap, cap), cap), :] = outbound[sp]

    def dispatch(k):
        out_copy(sp, lax.rem(sp + sp_count - k - 1, sp_count)).start()

    loop(sp_count - 1, dispatch)

    def at(k):
        return lax.rem(sp + k, sp_count)

    def counterpart(d):
        return lax.rem(chip + d, chips) * 2 + core

    def fan_first(k):
        s = at(k)

        @pl.when(k > 0)
        def _():
            out_copy(s, s).wait_recv()

        for d in range(1, chips):
            fan_copy(s, tp, counterpart(d), d - 1).start()
        fan_copy(s, tp, partner, chips - 1).start()

    def fan_second(k):
        s = at(k)
        for d in range(1, chips):
            source = counterpart(chips - d)
            fan_copy(s, source, source, 0).wait_recv()
            fan_copy(s, source, partner, chips - 1 + d).start()

    def pair_copy(s, a):
        return remote(
            block(partial_ref, s, a * 2 + 1 - core),
            pair_in.at[s, a],
            pair_send.at[s, a],
            pair_recv.at[s, a],
            {"tp": partner},
        )

    def cross_copy(s, a, slot):
        return remote(
            cross_out.at[s, a],
            cross_in.at[s, slot],
            cross_send.at[s, a],
            cross_recv.at[s, slot],
            {"tp": a * 2 + core},
        )

    def final_copy(s, slot):
        return remote(
            final_ref.at[s], returned.at[slot], final_send.at[s], final_recv.at[slot], {"sp": s}
        )

    def compute(k):
        s = at(k)
        for a in range(chips):
            t = a * 2 + 1 - core
            fan_copy(s, t, partner, 0).wait_recv()

        @pl.when(k == 0)
        def _():
            for copy in weights:
                copy.wait()

        x = rows[s]
        gate = jnp.dot(x, gate_ref[...], preferred_element_type=f32)
        up = jnp.dot(x, up_ref[...], preferred_element_type=f32)
        hidden = (gate / (1.0 + jnp.exp(-gate)) * up).astype(bf16)
        partial_ref[s] = jnp.dot(hidden, down_ref[...], preferred_element_type=f32).astype(bf16)
        for a in range(chips):
            pair_copy(s, a).start()

    def mine(s, a):
        t = a * 2 + core
        return partial_ref[s, pl.ds(pl.multiple_of(t * cap, cap), cap), :].astype(f32)

    def cross(k):
        s = at(k)
        for d in range(1, chips):
            a = lax.rem(chip + d, chips)
            pair_copy(s, a).wait_recv()
            cross_out[s, a] = (mine(s, a) + pair_in[s, a].astype(f32)).astype(bf16)
            cross_copy(s, a, chip).start()

    def finish(k):
        s = at(k)
        pair_copy(s, chip).wait_recv()
        total = mine(s, chip) + pair_in[s, chip].astype(f32)
        for d in range(1, chips):
            a = lax.rem(chip + d, chips)
            cross_copy(s, a, a).wait_recv()
            total = total + cross_in[s, a].astype(f32)
        final_ref[s] = total.astype(bf16)

        @pl.when(k > 0)
        def _():
            final_copy(s, sp).start()

    fan_first(0)
    if sp_count > 1:
        fan_first(1)
    fan_second(0)

    def turn(i):
        @pl.when(i + 1 < sp_count)
        def _():
            fan_second(i + 1)

        @pl.when(i < sp_count)
        def _():
            compute(i)

        @pl.when(i + 2 < sp_count)
        def _():
            fan_first(i + 2)

        @pl.when((i >= 1) & (i < sp_count + 1))
        def _():
            cross(i - 1)

        @pl.when(i >= 2)
        def _():
            finish(i - 2)

    loop(sp_count + 2, turn)

    returned[sp] = final_ref[sp]

    def collect(k):
        s = lax.rem(sp + sp_count - k - 1, sp_count)
        final_copy(s, s).wait_recv()

    loop(sp_count - 1, collect)
    picked = returned[...].reshape(sp_count * cap, returned.shape[2]).astype(f32)
    routed = jnp.dot(combine_ref[...], picked, precision=highest, preferred_element_type=f32)
    result_ref[...] = (stream_ref[...] + routed).astype(bf16)

    for k in range(1, tp_count):
        part_copy(tp, lax.rem(tp + k, tp_count)).wait_send()

    def drain(k):
        s = at(k)

        @pl.when(k > 0)
        def _():
            out_copy(sp, s).wait_send()
            final_copy(s, sp).wait_send()

        for d in range(1, chips):
            fan_copy(s, tp, counterpart(d), d - 1).wait_send()
            fan_copy(s, counterpart(chips - d), partner, chips - 1 + d).wait_send()
            a = lax.rem(chip + d, chips)
            cross_copy(s, a, chip).wait_send()
        fan_copy(s, tp, partner, chips - 1).wait_send()
        for a in range(chips):
            pair_copy(s, a).wait_send()

    loop(sp_count, drain)


def after_mixer(gated, out_weight, residual, gain, place, combine, gate_w, up_w, down_w, cap):
    sp_count, tp_count = lax.axis_size("sp"), lax.axis_size("tp")
    chips = tp_count // 2
    local, width = residual.shape
    bf16 = jnp.bfloat16
    vmem = pl.BlockSpec(memory_space=pltpu.VMEM)
    hbm = pl.BlockSpec(memory_space=pl.ANY)
    dma = pltpu.SemaphoreType.DMA
    return pl.pallas_call(
        partial(tail_kernel, sp_count, tp_count, cap),
        out_shape=jax.ShapeDtypeStruct((local, width), bf16),
        in_specs=[vmem] * 6 + [hbm] * 3,
        out_specs=vmem,
        scratch_shapes=[
            pltpu.VMEM(gate_w.shape[1:], bf16),
            pltpu.VMEM(up_w.shape[1:], bf16),
            pltpu.VMEM(down_w.shape[1:], bf16),
            pltpu.VMEM((tp_count, local, width), bf16),
            pltpu.VMEM((tp_count, local, width), bf16),
            pltpu.VMEM((local, width), jnp.float32),
            pltpu.VMEM((sp_count, cap, width), bf16),
            pltpu.VMEM((sp_count, tp_count * cap, width), bf16),
            pltpu.VMEM((sp_count, tp_count * cap, width), bf16),
            pltpu.VMEM((sp_count, chips, cap, width), bf16),
            pltpu.VMEM((sp_count, chips, cap, width), bf16),
            pltpu.VMEM((sp_count, chips, cap, width), bf16),
            pltpu.VMEM((sp_count, cap, width), bf16),
            pltpu.VMEM((sp_count, cap, width), bf16),
            dma((3,)),
            dma((tp_count,)),
            dma((tp_count,)),
            dma((sp_count,)),
            dma((sp_count,)),
            dma((sp_count, tp_count)),
            dma((sp_count, tp_count)),
            dma((sp_count, chips)),
            dma((sp_count, chips)),
            dma((sp_count, chips)),
            dma((sp_count, chips)),
            dma((sp_count,)),
            dma((sp_count,)),
        ],
        compiler_params=pltpu.CompilerParams(
            collective_id=0, has_side_effects=True, vmem_limit_bytes=60 * 1024 * 1024
        ),
    )(gated, out_weight, residual, gain, place, combine, gate_w, up_w, down_w)


def into_block_rows(array):
    blocks = array.shape[0] // BLK
    heads_here = array.shape[1] // HEAD
    return array.astype(jnp.float32).reshape(blocks, BLK, heads_here, HEAD).transpose(2, 0, 1, 3)


def square_product(first, second):
    return jnp.einsum("hij,hjk->hik", first, second, precision=highest)


def join_later(earlier, later):
    trans_a, state_a = earlier
    trans_b, state_b = later
    return (square_product(trans_a, trans_b), square_product(state_a, trans_b) + state_b)


def advance(carry, item):
    prod_now, state_now = carry
    trans_here, local_here = item
    return (
        (square_product(prod_now, trans_here), square_product(state_now, trans_here) + local_here),
        (prod_now, state_now),
    )


def body(
    receptance,
    head_keys,
    head_values,
    decay_logits,
    decay_boost,
    correction_logits,
    gate_logits,
    head_norm_gain,
    output_weight,
    residual,
    expert_norm_gain,
    routes,
    routing_weight,
    expert_gate_weight,
    expert_up_weight,
    expert_down_weight,
):
    length_here = receptance.shape[0]
    width_here = receptance.shape[1]
    query = into_block_rows(receptance)
    keyed = into_block_rows(head_keys)
    valued = into_block_rows(head_values)
    heads_here = query.shape[0]
    unit = keyed * lax.rsqrt(jnp.sum(keyed * keyed, axis=-1, keepdims=True) + 1e-06)
    rate = jax.nn.sigmoid(into_block_rows(correction_logits))
    decay_logarithm = -jnp.exp(
        -jax.nn.softplus(-into_block_rows(decay_logits)) - 0.5
    ) + into_block_rows(decay_boost)
    remove = -unit
    insert = unit * rate
    upto = jnp.cumsum(decay_logarithm, axis=2)
    before = upto - decay_logarithm
    final_log = upto[:, :, -1:, :]
    remove_scaled = remove * jnp.exp(before)
    query_scaled = query * jnp.exp(upto)
    insert_scaled = insert * jnp.exp(-upto)
    key_scaled = keyed * jnp.exp(-upto)
    position = jnp.arange(BLK)
    strict = (position[:, None] > position[None, :]).astype(jnp.float32)
    inclusive = (position[:, None] >= position[None, :]).astype(jnp.float32)
    pairwise = partial(jnp.einsum, "hntc,hnsc->hnts", precision=highest)
    apply_rows = partial(jnp.einsum, "hnts,hnsc->hntc", precision=highest)
    outer_sum = partial(jnp.einsum, "hnsi,hnsj->hnij", precision=highest)
    among = pairwise(remove_scaled, insert_scaled) * strict
    among_keys = pairwise(remove_scaled, key_scaled) * strict
    read_insert = pairwise(query_scaled, insert_scaled) * inclusive
    read_keys = pairwise(query_scaled, key_scaled) * inclusive
    solver = jnp.eye(BLK, dtype=jnp.float32) + among
    power = among
    covered = 1
    while covered < BLK - 1:
        power = apply_rows(power, power)
        solver = solver + apply_rows(solver, power)
        covered = 2 * covered + 1
    from_start = apply_rows(solver, remove_scaled)
    from_local = apply_rows(solver, apply_rows(among_keys, valued))
    query_map = query_scaled + apply_rows(read_insert, from_start)
    local_out = apply_rows(read_insert, from_local) + apply_rows(read_keys, valued)
    tail = jnp.exp(final_log - upto)
    insert_tail = insert * tail
    key_tail = keyed * tail
    eye_head = jnp.eye(HEAD, dtype=jnp.float32)
    block_trans = eye_head * jnp.exp(final_log) + outer_sum(from_start, insert_tail)
    block_state = outer_sum(from_local, insert_tail) + outer_sum(valued, key_tail)
    start = (
        jnp.broadcast_to(eye_head, (heads_here, HEAD, HEAD)),
        jnp.zeros((heads_here, HEAD, HEAD), jnp.float32),
    )
    (device_trans, device_state), (prefix_trans, prefix_state) = lax.scan(
        advance, start, (block_trans.transpose(1, 0, 2, 3), block_state.transpose(1, 0, 2, 3))
    )
    carried_query = jnp.einsum("hntk,nhjk->hntj", query_map, prefix_trans, precision=highest)
    own_out = local_out + jnp.einsum("hntk,nhvk->hntv", query_map, prefix_state, precision=highest)
    incoming = prefix((device_trans, device_state), "sp", join_later, start)
    mixed = own_out + jnp.einsum("hntk,hvk->hntv", carried_query, incoming[1], precision=highest)
    centre = mixed - jnp.mean(mixed, axis=-1, keepdims=True)
    spread = jnp.mean(centre * centre, axis=-1, keepdims=True)
    normed = centre * lax.rsqrt(spread + 0.00064) * head_norm_gain.reshape(heads_here, 1, 1, HEAD)
    normed = normed.transpose(1, 2, 0, 3).reshape(length_here, width_here)
    gated = (normed * jax.nn.sigmoid(gate_logits.astype(jnp.float32))).astype(jnp.bfloat16)
    sp_count = lax.axis_size("sp")
    tp_count = lax.axis_size("tp")
    capacity = max(2, 2 * TOK_DEV * TOP // (tp_count * sp_count))
    cap = -(-capacity // 16) * 16
    local_count = residual.shape[0]
    flat_routes = routes.reshape(-1)
    expert_ids = jnp.arange(sp_count, dtype=jnp.int32)
    chosen = (flat_routes[:, None] == expert_ids[None, :]).astype(jnp.int32)
    earlier = jnp.cumsum(chosen, axis=0) - chosen
    slot_index = jnp.sum(earlier * chosen, axis=1)
    target = flat_routes * cap + slot_index
    slots = jnp.arange(sp_count * cap, dtype=jnp.int32)
    placed = (target[:, None] == slots[None, :]).reshape(local_count, TOP, sp_count * cap)
    placed = placed.astype(jnp.float32)
    place = jnp.sum(placed, axis=1).astype(jnp.bfloat16).T
    combine = jnp.sum(placed * routing_weight[:, :, None], axis=1)
    return after_mixer(
        gated,
        output_weight,
        residual,
        expert_norm_gain[None, :],
        place,
        combine,
        expert_gate_weight,
        expert_up_weight,
        expert_down_weight,
        cap,
    )


def solution(mesh):
    placed = (
        P(("grp", "sp"), "tp"),
        P(("grp", "sp"), "tp"),
        P(("grp", "sp"), "tp"),
        P(("grp", "sp"), "tp"),
        P(("grp", "sp"), "tp"),
        P(("grp", "sp"), "tp"),
        P(("grp", "sp"), "tp"),
        P("tp"),
        P("tp", None),
        P(("grp", "sp", "tp"), None),
        P(),
        P(("grp", "sp", "tp"), None),
        P(("grp", "sp", "tp"), None),
        P("sp", None, "tp"),
        P("sp", None, "tp"),
        P("sp", "tp", None),
    )
    return jax.shard_map(
        body, mesh=mesh, in_specs=placed, out_specs=P(("grp", "sp", "tp"), None), check_vma=False
    )
```

```python
from functools import partial

import jax
import jax.numpy as jnp
from jax import lax
from jax.experimental import pallas as pl
from jax.experimental.pallas import tpu as pltpu
from jax.sharding import PartitionSpec as P

HEAD = 64
TOP = 2
BLK = 32
TOK_DEV = 128


highest = lax.Precision.HIGHEST


MESH = pl.DeviceIdType.MESH


def exact(first, second):
    return jnp.dot(first, second, precision=highest, preferred_element_type=jnp.float32)


def exact_rows(first, second):
    return lax.dot_general(
        first,
        second,
        (((1,), (1,)), ((), ())),
        precision=highest,
        preferred_element_type=jnp.float32,
    )


def carry_kernel(
    size,
    trans_ref,
    state_ref,
    query_ref,
    local_ref,
    mixed_ref,
    own_ref,
    all_ref,
    carried_ref,
    incoming_ref,
    send_sem,
    recv_sem,
):
    me = lax.axis_index("sp")
    heads, blocks = trans_ref.shape[0], trans_ref.shape[1]
    barrier = pltpu.get_barrier_semaphore()
    for k in range(1, size):
        peer = lax.rem(me + k, size)
        pl.semaphore_signal(barrier, inc=1, device_id={"sp": peer}, device_id_type=MESH)

    trans = [trans_ref[h, 0] for h in range(heads)]
    state = [state_ref[h, 0] for h in range(heads)]
    befores = []
    for n in range(1, blocks):
        befores.append((trans, state))
        step = [trans_ref[h, n] for h in range(heads)]
        trans = [exact(trans[h], step[h]) for h in range(heads)]
        state = [exact(state[h], step[h]) + state_ref[h, n] for h in range(heads)]
    for h in range(heads):
        own_ref[h] = jnp.concatenate([trans[h], state[h]], axis=-1).astype(jnp.bfloat16)
    incoming_ref[...] = jnp.zeros(incoming_ref.shape, jnp.float32)
    pl.semaphore_wait(barrier, size - 1)

    def transfer(slot, peer):
        return pltpu.make_async_remote_copy(
            src_ref=own_ref,
            dst_ref=all_ref.at[slot],
            send_sem=send_sem.at[peer],
            recv_sem=recv_sem.at[slot],
            device_id={"sp": peer},
            device_id_type=MESH,
        )

    def loop(action):
        def step(peer, carry):
            action(peer)
            return carry

        lax.fori_loop(0, size, step, 0)

    def send(peer):
        @pl.when(peer > me)
        def _():
            transfer(me, peer).start()

    def receive(peer):
        @pl.when(peer < me)
        def _():
            transfer(peer, peer).wait_recv()
            for h in range(heads):
                item = all_ref[peer, h].astype(jnp.float32)
                incoming_ref[h] = exact(incoming_ref[h], item[:, :HEAD]) + item[:, HEAD:]

    def finish(peer):
        @pl.when(peer > me)
        def _():
            transfer(me, peer).wait_send()

    loop(send)
    for h in range(heads):
        carried_ref[h, 0] = query_ref[h, 0]
        mixed_ref[h, 0] = local_ref[h, 0]
        for n in range(1, blocks):
            trans, state = befores[n - 1]
            carried_ref[h, n] = exact_rows(query_ref[h, n], trans[h])
            mixed_ref[h, n] = local_ref[h, n] + exact_rows(query_ref[h, n], state[h])
    loop(receive)
    for h in range(heads):
        for n in range(blocks):
            mixed_ref[h, n] = mixed_ref[h, n] + exact_rows(carried_ref[h, n], incoming_ref[h])
    loop(finish)


def carry(trans, state, query, local):
    size = lax.axis_size("sp")
    heads = trans.shape[0]
    vmem = pl.BlockSpec(memory_space=pltpu.VMEM)
    return pl.pallas_call(
        partial(carry_kernel, size),
        out_shape=jax.ShapeDtypeStruct(local.shape, jnp.float32),
        in_specs=[vmem] * 4,
        out_specs=vmem,
        scratch_shapes=[
            pltpu.VMEM((heads, HEAD, 2 * HEAD), jnp.bfloat16),
            pltpu.VMEM((size, heads, HEAD, 2 * HEAD), jnp.bfloat16),
            pltpu.VMEM(query.shape, jnp.float32),
            pltpu.VMEM((heads, HEAD, HEAD), jnp.float32),
            pltpu.SemaphoreType.DMA((size,)),
            pltpu.SemaphoreType.DMA((size,)),
        ],
        compiler_params=pltpu.CompilerParams(collective_id=1, has_side_effects=True),
    )(trans, state, query, local)


def tail_kernel(
    sp_count,
    tp_count,
    cap,
    gated_ref,
    out_weight_ref,
    residual_ref,
    gain_ref,
    place_ref,
    combine_ref,
    gate_hbm,
    up_hbm,
    down_hbm,
    result_ref,
    gate_ref,
    up_ref,
    down_ref,
    part,
    part_in,
    stream_ref,
    outbound,
    rows,
    partial_ref,
    pair_in,
    cross_out,
    cross_in,
    final_ref,
    returned,
    weight_sem,
    part_send,
    part_recv,
    out_send,
    out_recv,
    fan_send,
    row_recv,
    pair_send,
    pair_recv,
    cross_send,
    cross_recv,
    final_send,
    final_recv,
):
    sp, tp = lax.axis_index("sp"), lax.axis_index("tp")
    chips = tp_count // 2
    chip, core = tp // 2, lax.rem(tp, 2)
    partner = chip * 2 + 1 - core
    local = residual_ref.shape[0]
    f32, bf16 = jnp.float32, jnp.bfloat16

    weights = [
        pltpu.make_async_copy(source.at[0], target, weight_sem.at[n])
        for n, (source, target) in enumerate(
            ((gate_hbm, gate_ref), (up_hbm, up_ref), (down_hbm, down_ref))
        )
    ]
    for copy in weights:
        copy.start()

    barrier = pltpu.get_barrier_semaphore()
    for k in range(1, sp_count):
        peer = lax.rem(sp + k, sp_count)
        pl.semaphore_signal(barrier, inc=1, device_id={"sp": peer}, device_id_type=MESH)
    for k in range(1, tp_count):
        peer = lax.rem(tp + k, tp_count)
        pl.semaphore_signal(barrier, inc=1, device_id={"tp": peer}, device_id_type=MESH)
    pl.semaphore_wait(barrier, sp_count + tp_count - 2)

    def remote(source, target, send, recv, where):
        return pltpu.make_async_remote_copy(
            src_ref=source,
            dst_ref=target,
            send_sem=send,
            recv_sem=recv,
            device_id=where,
            device_id_type=MESH,
        )

    def loop(count, action):
        def step(k, carry):
            action(k)
            return carry

        lax.fori_loop(0, count, step, 0)

    def part_copy(slot, peer):
        return remote(
            part.at[peer], part_in.at[slot], part_send.at[peer], part_recv.at[slot], {"tp": peer}
        )

    for k in range(1, tp_count + 1):
        peer = lax.rem(tp + k, tp_count)
        piece = gated_ref[pl.ds(pl.multiple_of(peer * local, local), local), :]
        part[peer] = jnp.dot(piece, out_weight_ref[...], preferred_element_type=f32).astype(bf16)
        if k < tp_count:
            part_copy(tp, peer).start()
    stream = residual_ref[...].astype(f32) + part[tp].astype(f32)
    for k in range(1, tp_count):
        peer = lax.rem(tp + tp_count - k, tp_count)
        part_copy(peer, peer).wait_recv()
        stream = stream + part_in[peer].astype(f32)
    stream_ref[...] = stream
    normal = (
        stream
        * lax.rsqrt(jnp.mean(stream * stream, axis=-1, keepdims=True) + 1e-06)
        * gain_ref[...]
    ).astype(bf16)
    sent = jnp.dot(place_ref[...], normal, preferred_element_type=f32).astype(bf16)
    outbound[...] = sent.reshape(outbound.shape)

    def block(ref, s, t):
        return ref.at[s, pl.ds(pl.multiple_of(t * cap, cap), cap)]

    def out_copy(slot, peer):
        return remote(
            outbound.at[peer],
            block(rows, slot, tp),
            out_send.at[peer],
            out_recv.at[slot],
            {"sp": peer},
        )

    def own_block(s):
        return block(rows, s, tp)

    def fan_copy(s, t, peer, slot):
        return remote(
            block(rows, s, t),
            block(rows, s, t),
            fan_send.at[s, slot],
            row_recv.at[s, t],
            {"tp": peer},
        )

    rows[sp, pl.ds(pl.multiple_of(tp * cap, cap), cap), :] = outbound[sp]

    def dispatch(k):
        out_copy(sp, lax.rem(sp + sp_count - k - 1, sp_count)).start()

    loop(sp_count - 1, dispatch)

    def at(k):
        return lax.rem(sp + k, sp_count)

    def counterpart(d):
        return lax.rem(chip + d, chips) * 2 + core

    def fan_first(k):
        s = at(k)

        @pl.when(k > 0)
        def _():
            out_copy(s, s).wait_recv()

        for d in range(1, chips):
            fan_copy(s, tp, counterpart(d), d - 1).start()
        fan_copy(s, tp, partner, chips - 1).start()

    def fan_second(k):
        s = at(k)
        for d in range(1, chips):
            source = counterpart(chips - d)
            fan_copy(s, source, source, 0).wait_recv()
            fan_copy(s, source, partner, chips - 1 + d).start()

    def pair_copy(s, a):
        return remote(
            block(partial_ref, s, a * 2 + 1 - core),
            pair_in.at[s, a],
            pair_send.at[s, a],
            pair_recv.at[s, a],
            {"tp": partner},
        )

    def cross_copy(s, a, slot):
        return remote(
            cross_out.at[s, a],
            cross_in.at[s, slot],
            cross_send.at[s, a],
            cross_recv.at[s, slot],
            {"tp": a * 2 + core},
        )

    def final_copy(s, slot):
        return remote(
            final_ref.at[s], returned.at[slot], final_send.at[s], final_recv.at[slot], {"sp": s}
        )

    def compute(k):
        s = at(k)
        for a in range(chips):
            t = a * 2 + 1 - core
            fan_copy(s, t, partner, 0).wait_recv()

        @pl.when(k == 0)
        def _():
            for copy in weights:
                copy.wait()

        x = rows[s]
        gate = jnp.dot(x, gate_ref[...], preferred_element_type=f32)
        up = jnp.dot(x, up_ref[...], preferred_element_type=f32)
        hidden = (gate / (1.0 + jnp.exp(-gate)) * up).astype(bf16)
        partial_ref[s] = jnp.dot(hidden, down_ref[...], preferred_element_type=f32).astype(bf16)
        for a in range(chips):
            pair_copy(s, a).start()

    def mine(s, a):
        t = a * 2 + core
        return partial_ref[s, pl.ds(pl.multiple_of(t * cap, cap), cap), :].astype(f32)

    def cross(k):
        s = at(k)
        for d in range(1, chips):
            a = lax.rem(chip + d, chips)
            pair_copy(s, a).wait_recv()
            cross_out[s, a] = (mine(s, a) + pair_in[s, a].astype(f32)).astype(bf16)
            cross_copy(s, a, chip).start()

    def finish(k):
        s = at(k)
        pair_copy(s, chip).wait_recv()
        total = mine(s, chip) + pair_in[s, chip].astype(f32)
        for d in range(1, chips):
            a = lax.rem(chip + d, chips)
            cross_copy(s, a, a).wait_recv()
            total = total + cross_in[s, a].astype(f32)
        final_ref[s] = total.astype(bf16)

        @pl.when(k > 0)
        def _():
            final_copy(s, sp).start()

    fan_first(0)
    if sp_count > 1:
        fan_first(1)
    fan_second(0)

    def turn(i):
        @pl.when(i + 1 < sp_count)
        def _():
            fan_second(i + 1)

        @pl.when(i < sp_count)
        def _():
            compute(i)

        @pl.when(i + 2 < sp_count)
        def _():
            fan_first(i + 2)

        @pl.when((i >= 1) & (i < sp_count + 1))
        def _():
            cross(i - 1)

        @pl.when(i >= 2)
        def _():
            finish(i - 2)

    loop(sp_count + 2, turn)

    returned[sp] = final_ref[sp]

    def collect(k):
        s = lax.rem(sp + sp_count - k - 1, sp_count)
        final_copy(s, s).wait_recv()

    loop(sp_count - 1, collect)
    picked = returned[...].reshape(sp_count * cap, returned.shape[2]).astype(f32)
    routed = jnp.dot(combine_ref[...], picked, precision=highest, preferred_element_type=f32)
    result_ref[...] = (stream_ref[...] + routed).astype(bf16)

    for k in range(1, tp_count):
        part_copy(tp, lax.rem(tp + k, tp_count)).wait_send()

    def drain(k):
        s = at(k)

        @pl.when(k > 0)
        def _():
            out_copy(sp, s).wait_send()
            final_copy(s, sp).wait_send()

        for d in range(1, chips):
            fan_copy(s, tp, counterpart(d), d - 1).wait_send()
            fan_copy(s, counterpart(chips - d), partner, chips - 1 + d).wait_send()
            a = lax.rem(chip + d, chips)
            cross_copy(s, a, chip).wait_send()
        fan_copy(s, tp, partner, chips - 1).wait_send()
        for a in range(chips):
            pair_copy(s, a).wait_send()

    loop(sp_count, drain)


def after_mixer(gated, out_weight, residual, gain, place, combine, gate_w, up_w, down_w, cap):
    sp_count, tp_count = lax.axis_size("sp"), lax.axis_size("tp")
    chips = tp_count // 2
    local, width = residual.shape
    bf16 = jnp.bfloat16
    vmem = pl.BlockSpec(memory_space=pltpu.VMEM)
    hbm = pl.BlockSpec(memory_space=pl.ANY)
    dma = pltpu.SemaphoreType.DMA
    return pl.pallas_call(
        partial(tail_kernel, sp_count, tp_count, cap),
        out_shape=jax.ShapeDtypeStruct((local, width), bf16),
        in_specs=[vmem] * 6 + [hbm] * 3,
        out_specs=vmem,
        scratch_shapes=[
            pltpu.VMEM(gate_w.shape[1:], bf16),
            pltpu.VMEM(up_w.shape[1:], bf16),
            pltpu.VMEM(down_w.shape[1:], bf16),
            pltpu.VMEM((tp_count, local, width), bf16),
            pltpu.VMEM((tp_count, local, width), bf16),
            pltpu.VMEM((local, width), jnp.float32),
            pltpu.VMEM((sp_count, cap, width), bf16),
            pltpu.VMEM((sp_count, tp_count * cap, width), bf16),
            pltpu.VMEM((sp_count, tp_count * cap, width), bf16),
            pltpu.VMEM((sp_count, chips, cap, width), bf16),
            pltpu.VMEM((sp_count, chips, cap, width), bf16),
            pltpu.VMEM((sp_count, chips, cap, width), bf16),
            pltpu.VMEM((sp_count, cap, width), bf16),
            pltpu.VMEM((sp_count, cap, width), bf16),
            dma((3,)),
            dma((tp_count,)),
            dma((tp_count,)),
            dma((sp_count,)),
            dma((sp_count,)),
            dma((sp_count, tp_count)),
            dma((sp_count, tp_count)),
            dma((sp_count, chips)),
            dma((sp_count, chips)),
            dma((sp_count, chips)),
            dma((sp_count, chips)),
            dma((sp_count,)),
            dma((sp_count,)),
        ],
        compiler_params=pltpu.CompilerParams(
            collective_id=0, has_side_effects=True, vmem_limit_bytes=60 * 1024 * 1024
        ),
    )(gated, out_weight, residual, gain, place, combine, gate_w, up_w, down_w)


def into_block_rows(array):
    blocks = array.shape[0] // BLK
    heads_here = array.shape[1] // HEAD
    return array.astype(jnp.float32).reshape(blocks, BLK, heads_here, HEAD).transpose(2, 0, 1, 3)


def body(
    receptance,
    head_keys,
    head_values,
    decay_logits,
    decay_boost,
    correction_logits,
    gate_logits,
    head_norm_gain,
    output_weight,
    residual,
    expert_norm_gain,
    routes,
    routing_weight,
    expert_gate_weight,
    expert_up_weight,
    expert_down_weight,
):
    length_here = receptance.shape[0]
    width_here = receptance.shape[1]
    query = into_block_rows(receptance)
    keyed = into_block_rows(head_keys)
    valued = into_block_rows(head_values)
    heads_here = query.shape[0]
    unit = keyed * lax.rsqrt(jnp.sum(keyed * keyed, axis=-1, keepdims=True) + 1e-06)
    rate = jax.nn.sigmoid(into_block_rows(correction_logits))
    decay_logarithm = -jnp.exp(
        -jax.nn.softplus(-into_block_rows(decay_logits)) - 0.5
    ) + into_block_rows(decay_boost)
    remove = -unit
    insert = unit * rate
    upto = jnp.cumsum(decay_logarithm, axis=2)
    before = upto - decay_logarithm
    final_log = upto[:, :, -1:, :]
    remove_scaled = remove * jnp.exp(before)
    query_scaled = query * jnp.exp(upto)
    insert_scaled = insert * jnp.exp(-upto)
    key_scaled = keyed * jnp.exp(-upto)
    position = jnp.arange(BLK)
    strict = (position[:, None] > position[None, :]).astype(jnp.float32)
    inclusive = (position[:, None] >= position[None, :]).astype(jnp.float32)
    pairwise = partial(jnp.einsum, "hntc,hnsc->hnts", precision=highest)
    apply_rows = partial(jnp.einsum, "hnts,hnsc->hntc", precision=highest)
    outer_sum = partial(jnp.einsum, "hnsi,hnsj->hnij", precision=highest)
    among = pairwise(remove_scaled, insert_scaled) * strict
    among_keys = pairwise(remove_scaled, key_scaled) * strict
    read_insert = pairwise(query_scaled, insert_scaled) * inclusive
    read_keys = pairwise(query_scaled, key_scaled) * inclusive
    solver = jnp.eye(BLK, dtype=jnp.float32) + among
    power = among
    covered = 1
    while covered < BLK - 1:
        power = apply_rows(power, power)
        solver = solver + apply_rows(solver, power)
        covered = 2 * covered + 1
    from_start = apply_rows(solver, remove_scaled)
    from_local = apply_rows(solver, apply_rows(among_keys, valued))
    query_map = query_scaled + apply_rows(read_insert, from_start)
    local_out = apply_rows(read_insert, from_local) + apply_rows(read_keys, valued)
    tail = jnp.exp(final_log - upto)
    insert_tail = insert * tail
    key_tail = keyed * tail
    eye_head = jnp.eye(HEAD, dtype=jnp.float32)
    block_trans = eye_head * jnp.exp(final_log) + outer_sum(from_start, insert_tail)
    block_state = outer_sum(from_local, insert_tail) + outer_sum(valued, key_tail)
    mixed = carry(block_trans, block_state, query_map, local_out)
    centre = mixed - jnp.mean(mixed, axis=-1, keepdims=True)
    spread = jnp.mean(centre * centre, axis=-1, keepdims=True)
    normed = centre * lax.rsqrt(spread + 0.00064) * head_norm_gain.reshape(heads_here, 1, 1, HEAD)
    normed = normed.transpose(1, 2, 0, 3).reshape(length_here, width_here)
    gated = (normed * jax.nn.sigmoid(gate_logits.astype(jnp.float32))).astype(jnp.bfloat16)
    sp_count = lax.axis_size("sp")
    tp_count = lax.axis_size("tp")
    capacity = max(2, 2 * TOK_DEV * TOP // (tp_count * sp_count))
    cap = -(-capacity // 16) * 16
    local_count = residual.shape[0]
    flat_routes = routes.reshape(-1)
    expert_ids = jnp.arange(sp_count, dtype=jnp.int32)
    chosen = (flat_routes[:, None] == expert_ids[None, :]).astype(jnp.int32)
    earlier = jnp.cumsum(chosen, axis=0) - chosen
    slot_index = jnp.sum(earlier * chosen, axis=1)
    target = flat_routes * cap + slot_index
    slots = jnp.arange(sp_count * cap, dtype=jnp.int32)
    placed = (target[:, None] == slots[None, :]).reshape(local_count, TOP, sp_count * cap)
    placed = placed.astype(jnp.float32)
    place = jnp.sum(placed, axis=1).astype(jnp.bfloat16).T
    combine = jnp.sum(placed * routing_weight[:, :, None], axis=1)
    return after_mixer(
        gated,
        output_weight,
        residual,
        expert_norm_gain[None, :],
        place,
        combine,
        expert_gate_weight,
        expert_up_weight,
        expert_down_weight,
        cap,
    )


def solution(mesh):
    placed = (
        P(("grp", "sp"), "tp"),
        P(("grp", "sp"), "tp"),
        P(("grp", "sp"), "tp"),
        P(("grp", "sp"), "tp"),
        P(("grp", "sp"), "tp"),
        P(("grp", "sp"), "tp"),
        P(("grp", "sp"), "tp"),
        P("tp"),
        P("tp", None),
        P(("grp", "sp", "tp"), None),
        P(),
        P(("grp", "sp", "tp"), None),
        P(("grp", "sp", "tp"), None),
        P("sp", None, "tp"),
        P("sp", None, "tp"),
        P("sp", "tp", None),
    )
    return jax.shard_map(
        body, mesh=mesh, in_specs=placed, out_specs=P(("grp", "sp", "tp"), None), check_vma=False
    )
```

```python
from functools import partial

import jax
import jax.numpy as jnp
from jax import lax
from jax.experimental import pallas as pl
from jax.experimental.pallas import tpu as pltpu
from jax.sharding import PartitionSpec as P

HEAD = 64
TOP = 2
BLK = 32
TOK_DEV = 128


highest = lax.Precision.HIGHEST


MESH = pl.DeviceIdType.MESH


def exact(first, second):
    return jnp.dot(first, second, precision=highest, preferred_element_type=jnp.float32)


def exact_rows(first, second):
    return lax.dot_general(
        first,
        second,
        (((1,), (1,)), ((), ())),
        precision=highest,
        preferred_element_type=jnp.float32,
    )


def carry_kernel(
    size,
    trans_ref,
    state_ref,
    query_ref,
    local_ref,
    mixed_ref,
    own_ref,
    all_ref,
    carried_ref,
    incoming_ref,
    send_sem,
    recv_sem,
):
    me = lax.axis_index("sp")
    heads, blocks = trans_ref.shape[0], trans_ref.shape[1]
    barrier = pltpu.get_barrier_semaphore()
    for k in range(1, size):
        peer = lax.rem(me + k, size)
        pl.semaphore_signal(barrier, inc=1, device_id={"sp": peer}, device_id_type=MESH)

    trans = [trans_ref[h, 0] for h in range(heads)]
    state = [state_ref[h, 0] for h in range(heads)]
    befores = []
    for n in range(1, blocks):
        befores.append((trans, state))
        step = [trans_ref[h, n] for h in range(heads)]
        trans = [exact(trans[h], step[h]) for h in range(heads)]
        state = [exact(state[h], step[h]) + state_ref[h, n] for h in range(heads)]
    for h in range(heads):
        own_ref[h] = jnp.concatenate([trans[h], state[h]], axis=-1).astype(jnp.bfloat16)
    incoming_ref[...] = jnp.zeros(incoming_ref.shape, jnp.float32)
    pl.semaphore_wait(barrier, size - 1)

    def transfer(slot, peer):
        return pltpu.make_async_remote_copy(
            src_ref=own_ref,
            dst_ref=all_ref.at[slot],
            send_sem=send_sem.at[peer],
            recv_sem=recv_sem.at[slot],
            device_id={"sp": peer},
            device_id_type=MESH,
        )

    def loop(action):
        def step(peer, carry):
            action(peer)
            return carry

        lax.fori_loop(0, size, step, 0)

    def send(peer):
        @pl.when(peer > me)
        def _():
            transfer(me, peer).start()

    def receive(peer):
        @pl.when(peer < me)
        def _():
            transfer(peer, peer).wait_recv()
            for h in range(heads):
                item = all_ref[peer, h].astype(jnp.float32)
                incoming_ref[h] = exact(incoming_ref[h], item[:, :HEAD]) + item[:, HEAD:]

    def finish(peer):
        @pl.when(peer > me)
        def _():
            transfer(me, peer).wait_send()

    loop(send)
    for h in range(heads):
        carried_ref[h, 0] = query_ref[h, 0]
        mixed_ref[h, 0] = local_ref[h, 0]
        for n in range(1, blocks):
            trans, state = befores[n - 1]
            carried_ref[h, n] = exact_rows(query_ref[h, n], trans[h])
            mixed_ref[h, n] = local_ref[h, n] + exact_rows(query_ref[h, n], state[h])
    loop(receive)
    for h in range(heads):
        for n in range(blocks):
            mixed_ref[h, n] = mixed_ref[h, n] + exact_rows(carried_ref[h, n], incoming_ref[h])
    loop(finish)


def carry(trans, state, query, local):
    size = lax.axis_size("sp")
    heads = trans.shape[0]
    vmem = pl.BlockSpec(memory_space=pltpu.VMEM)
    return pl.pallas_call(
        partial(carry_kernel, size),
        out_shape=jax.ShapeDtypeStruct(local.shape, jnp.float32),
        in_specs=[vmem] * 4,
        out_specs=vmem,
        scratch_shapes=[
            pltpu.VMEM((heads, HEAD, 2 * HEAD), jnp.bfloat16),
            pltpu.VMEM((size, heads, HEAD, 2 * HEAD), jnp.bfloat16),
            pltpu.VMEM(query.shape, jnp.float32),
            pltpu.VMEM((heads, HEAD, HEAD), jnp.float32),
            pltpu.SemaphoreType.DMA((size,)),
            pltpu.SemaphoreType.DMA((size,)),
        ],
        compiler_params=pltpu.CompilerParams(collective_id=1, has_side_effects=True),
    )(trans, state, query, local)


def tail_kernel(
    sp_count,
    tp_count,
    cap,
    gated_ref,
    out_weight_ref,
    residual_ref,
    gain_ref,
    place_ref,
    combine_ref,
    gate_hbm,
    up_hbm,
    down_hbm,
    result_ref,
    gate_ref,
    up_ref,
    down_ref,
    part,
    part_in,
    stream_ref,
    outbound,
    rows,
    partial_ref,
    pair_in,
    cross_out,
    cross_in,
    final_ref,
    returned,
    weight_sem,
    part_send,
    part_recv,
    out_send,
    out_recv,
    fan_send,
    row_recv,
    pair_send,
    pair_recv,
    cross_send,
    cross_recv,
    final_send,
    final_recv,
):
    sp, tp = lax.axis_index("sp"), lax.axis_index("tp")
    chips = tp_count // 2
    chip, core = tp // 2, lax.rem(tp, 2)
    partner = chip * 2 + 1 - core
    local = residual_ref.shape[0]
    f32, bf16 = jnp.float32, jnp.bfloat16

    weights = [
        pltpu.make_async_copy(source.at[0], target, weight_sem.at[n])
        for n, (source, target) in enumerate(
            ((gate_hbm, gate_ref), (up_hbm, up_ref), (down_hbm, down_ref))
        )
    ]
    for copy in weights:
        copy.start()

    barrier = pltpu.get_barrier_semaphore()
    for k in range(1, sp_count):
        peer = lax.rem(sp + k, sp_count)
        pl.semaphore_signal(barrier, inc=1, device_id={"sp": peer}, device_id_type=MESH)
    for k in range(1, tp_count):
        peer = lax.rem(tp + k, tp_count)
        pl.semaphore_signal(barrier, inc=1, device_id={"tp": peer}, device_id_type=MESH)
    pl.semaphore_wait(barrier, sp_count + tp_count - 2)

    def remote(source, target, send, recv, where):
        return pltpu.make_async_remote_copy(
            src_ref=source,
            dst_ref=target,
            send_sem=send,
            recv_sem=recv,
            device_id=where,
            device_id_type=MESH,
        )

    def loop(count, action):
        def step(k, carry):
            action(k)
            return carry

        lax.fori_loop(0, count, step, 0)

    def part_copy(slot, peer):
        return remote(
            part.at[peer], part_in.at[slot], part_send.at[peer], part_recv.at[slot], {"tp": peer}
        )

    for k in range(1, tp_count + 1):
        peer = lax.rem(tp + k, tp_count)
        piece = gated_ref[pl.ds(pl.multiple_of(peer * local, local), local), :]
        part[peer] = jnp.dot(piece, out_weight_ref[...], preferred_element_type=f32).astype(bf16)
        if k < tp_count:
            part_copy(tp, peer).start()
    stream = residual_ref[...].astype(f32) + part[tp].astype(f32)
    for k in range(1, tp_count):
        peer = lax.rem(tp + tp_count - k, tp_count)
        part_copy(peer, peer).wait_recv()
        stream = stream + part_in[peer].astype(f32)
    stream_ref[...] = stream
    normal = (
        stream
        * lax.rsqrt(jnp.mean(stream * stream, axis=-1, keepdims=True) + 1e-06)
        * gain_ref[...]
    ).astype(bf16)
    sent = jnp.dot(place_ref[...], normal, preferred_element_type=f32).astype(bf16)
    outbound[...] = sent.reshape(outbound.shape)

    def block(ref, s, t):
        return ref.at[s, pl.ds(pl.multiple_of(t * cap, cap), cap)]

    def out_copy(slot, peer):
        return remote(
            outbound.at[peer],
            block(rows, slot, tp),
            out_send.at[peer],
            out_recv.at[slot],
            {"sp": peer},
        )

    def own_block(s):
        return block(rows, s, tp)

    def fan_copy(s, t, peer, slot):
        return remote(
            block(rows, s, t),
            block(rows, s, t),
            fan_send.at[s, slot],
            row_recv.at[s, t],
            {"tp": peer},
        )

    rows[sp, pl.ds(pl.multiple_of(tp * cap, cap), cap), :] = outbound[sp]

    def dispatch(k):
        out_copy(sp, lax.rem(sp + sp_count - k - 1, sp_count)).start()

    loop(sp_count - 1, dispatch)

    def at(k):
        return lax.rem(sp + k, sp_count)

    def counterpart(d):
        return lax.rem(chip + d, chips) * 2 + core

    def fan_first(k):
        s = at(k)

        @pl.when(k > 0)
        def _():
            out_copy(s, s).wait_recv()

        for d in range(1, chips):
            fan_copy(s, tp, counterpart(d), d - 1).start()
        fan_copy(s, tp, partner, chips - 1).start()

    def fan_second(k):
        s = at(k)
        for d in range(1, chips):
            source = counterpart(chips - d)
            fan_copy(s, source, source, 0).wait_recv()
            fan_copy(s, source, partner, chips - 1 + d).start()

    def pair_copy(s, a):
        return remote(
            block(partial_ref, s, a * 2 + 1 - core),
            pair_in.at[s, a],
            pair_send.at[s, a],
            pair_recv.at[s, a],
            {"tp": partner},
        )

    def cross_copy(s, a, slot):
        return remote(
            cross_out.at[s, a],
            cross_in.at[s, slot],
            cross_send.at[s, a],
            cross_recv.at[s, slot],
            {"tp": a * 2 + core},
        )

    def final_copy(s, slot):
        return remote(
            final_ref.at[s], returned.at[slot], final_send.at[s], final_recv.at[slot], {"sp": s}
        )

    def compute(k):
        s = at(k)
        for a in range(chips):
            t = a * 2 + 1 - core
            fan_copy(s, t, partner, 0).wait_recv()

        @pl.when(k == 0)
        def _():
            for copy in weights:
                copy.wait()

        x = rows[s]
        gate = jnp.dot(x, gate_ref[...], preferred_element_type=f32)
        up = jnp.dot(x, up_ref[...], preferred_element_type=f32)
        hidden = (gate / (1.0 + jnp.exp(-gate)) * up).astype(bf16)
        partial_ref[s] = jnp.dot(hidden, down_ref[...], preferred_element_type=f32).astype(bf16)
        for a in range(chips):
            pair_copy(s, a).start()

    def mine(s, a):
        t = a * 2 + core
        return partial_ref[s, pl.ds(pl.multiple_of(t * cap, cap), cap), :].astype(f32)

    def cross(k):
        s = at(k)
        for d in range(1, chips):
            a = lax.rem(chip + d, chips)
            pair_copy(s, a).wait_recv()
            cross_out[s, a] = (mine(s, a) + pair_in[s, a].astype(f32)).astype(bf16)
            cross_copy(s, a, chip).start()

    def finish(k):
        s = at(k)
        pair_copy(s, chip).wait_recv()
        total = mine(s, chip) + pair_in[s, chip].astype(f32)
        for d in range(1, chips):
            a = lax.rem(chip + d, chips)
            cross_copy(s, a, a).wait_recv()
            total = total + cross_in[s, a].astype(f32)
        final_ref[s] = total.astype(bf16)

        @pl.when(k > 0)
        def _():
            final_copy(s, sp).start()

    fan_first(0)
    fan_second(0)
    if sp_count > 1:
        fan_first(1)

    def turn(i):
        @pl.when(i < sp_count)
        def _():
            compute(i)

        @pl.when(i + 1 < sp_count)
        def _():
            fan_second(i + 1)

        @pl.when(i + 2 < sp_count)
        def _():
            fan_first(i + 2)

        @pl.when((i >= 1) & (i < sp_count + 1))
        def _():
            cross(i - 1)

        @pl.when(i >= 2)
        def _():
            finish(i - 2)

    loop(sp_count + 2, turn)

    returned[sp] = final_ref[sp]

    def collect(k):
        s = lax.rem(sp + sp_count - k - 1, sp_count)
        final_copy(s, s).wait_recv()

    loop(sp_count - 1, collect)
    picked = returned[...].reshape(sp_count * cap, returned.shape[2]).astype(f32)
    routed = jnp.dot(combine_ref[...], picked, precision=highest, preferred_element_type=f32)
    result_ref[...] = (stream_ref[...] + routed).astype(bf16)

    for k in range(1, tp_count):
        part_copy(tp, lax.rem(tp + k, tp_count)).wait_send()

    def drain(k):
        s = at(k)

        @pl.when(k > 0)
        def _():
            out_copy(sp, s).wait_send()
            final_copy(s, sp).wait_send()

        for d in range(1, chips):
            fan_copy(s, tp, counterpart(d), d - 1).wait_send()
            fan_copy(s, counterpart(chips - d), partner, chips - 1 + d).wait_send()
            a = lax.rem(chip + d, chips)
            cross_copy(s, a, chip).wait_send()
        fan_copy(s, tp, partner, chips - 1).wait_send()
        for a in range(chips):
            pair_copy(s, a).wait_send()

    loop(sp_count, drain)


def after_mixer(gated, out_weight, residual, gain, place, combine, gate_w, up_w, down_w, cap):
    sp_count, tp_count = lax.axis_size("sp"), lax.axis_size("tp")
    chips = tp_count // 2
    local, width = residual.shape
    bf16 = jnp.bfloat16
    vmem = pl.BlockSpec(memory_space=pltpu.VMEM)
    hbm = pl.BlockSpec(memory_space=pl.ANY)
    dma = pltpu.SemaphoreType.DMA
    return pl.pallas_call(
        partial(tail_kernel, sp_count, tp_count, cap),
        out_shape=jax.ShapeDtypeStruct((local, width), bf16),
        in_specs=[vmem] * 6 + [hbm] * 3,
        out_specs=vmem,
        scratch_shapes=[
            pltpu.VMEM(gate_w.shape[1:], bf16),
            pltpu.VMEM(up_w.shape[1:], bf16),
            pltpu.VMEM(down_w.shape[1:], bf16),
            pltpu.VMEM((tp_count, local, width), bf16),
            pltpu.VMEM((tp_count, local, width), bf16),
            pltpu.VMEM((local, width), jnp.float32),
            pltpu.VMEM((sp_count, cap, width), bf16),
            pltpu.VMEM((sp_count, tp_count * cap, width), bf16),
            pltpu.VMEM((sp_count, tp_count * cap, width), bf16),
            pltpu.VMEM((sp_count, chips, cap, width), bf16),
            pltpu.VMEM((sp_count, chips, cap, width), bf16),
            pltpu.VMEM((sp_count, chips, cap, width), bf16),
            pltpu.VMEM((sp_count, cap, width), bf16),
            pltpu.VMEM((sp_count, cap, width), bf16),
            dma((3,)),
            dma((tp_count,)),
            dma((tp_count,)),
            dma((sp_count,)),
            dma((sp_count,)),
            dma((sp_count, tp_count)),
            dma((sp_count, tp_count)),
            dma((sp_count, chips)),
            dma((sp_count, chips)),
            dma((sp_count, chips)),
            dma((sp_count, chips)),
            dma((sp_count,)),
            dma((sp_count,)),
        ],
        compiler_params=pltpu.CompilerParams(
            collective_id=0, has_side_effects=True, vmem_limit_bytes=60 * 1024 * 1024
        ),
    )(gated, out_weight, residual, gain, place, combine, gate_w, up_w, down_w)


def into_block_rows(array):
    blocks = array.shape[0] // BLK
    heads_here = array.shape[1] // HEAD
    return array.astype(jnp.float32).reshape(blocks, BLK, heads_here, HEAD).transpose(2, 0, 1, 3)


def body(
    receptance,
    head_keys,
    head_values,
    decay_logits,
    decay_boost,
    correction_logits,
    gate_logits,
    head_norm_gain,
    output_weight,
    residual,
    expert_norm_gain,
    routes,
    routing_weight,
    expert_gate_weight,
    expert_up_weight,
    expert_down_weight,
):
    length_here = receptance.shape[0]
    width_here = receptance.shape[1]
    query = into_block_rows(receptance)
    keyed = into_block_rows(head_keys)
    valued = into_block_rows(head_values)
    heads_here = query.shape[0]
    unit = keyed * lax.rsqrt(jnp.sum(keyed * keyed, axis=-1, keepdims=True) + 1e-06)
    rate = jax.nn.sigmoid(into_block_rows(correction_logits))
    decay_logarithm = -jnp.exp(
        -jax.nn.softplus(-into_block_rows(decay_logits)) - 0.5
    ) + into_block_rows(decay_boost)
    remove = -unit
    insert = unit * rate
    upto = jnp.cumsum(decay_logarithm, axis=2)
    before = upto - decay_logarithm
    final_log = upto[:, :, -1:, :]
    remove_scaled = remove * jnp.exp(before)
    query_scaled = query * jnp.exp(upto)
    insert_scaled = insert * jnp.exp(-upto)
    key_scaled = keyed * jnp.exp(-upto)
    position = jnp.arange(BLK)
    strict = (position[:, None] > position[None, :]).astype(jnp.float32)
    inclusive = (position[:, None] >= position[None, :]).astype(jnp.float32)
    pairwise = partial(jnp.einsum, "hntc,hnsc->hnts", precision=highest)
    apply_rows = partial(jnp.einsum, "hnts,hnsc->hntc", precision=highest)
    outer_sum = partial(jnp.einsum, "hnsi,hnsj->hnij", precision=highest)
    among = pairwise(remove_scaled, insert_scaled) * strict
    among_keys = pairwise(remove_scaled, key_scaled) * strict
    read_insert = pairwise(query_scaled, insert_scaled) * inclusive
    read_keys = pairwise(query_scaled, key_scaled) * inclusive
    solver = jnp.eye(BLK, dtype=jnp.float32) + among
    power = among
    covered = 1
    while covered < BLK - 1:
        power = apply_rows(power, power)
        solver = solver + apply_rows(solver, power)
        covered = 2 * covered + 1
    from_start = apply_rows(solver, remove_scaled)
    from_local = apply_rows(solver, apply_rows(among_keys, valued))
    query_map = query_scaled + apply_rows(read_insert, from_start)
    local_out = apply_rows(read_insert, from_local) + apply_rows(read_keys, valued)
    tail = jnp.exp(final_log - upto)
    insert_tail = insert * tail
    key_tail = keyed * tail
    eye_head = jnp.eye(HEAD, dtype=jnp.float32)
    block_trans = eye_head * jnp.exp(final_log) + outer_sum(from_start, insert_tail)
    block_state = outer_sum(from_local, insert_tail) + outer_sum(valued, key_tail)
    mixed = carry(block_trans, block_state, query_map, local_out)
    centre = mixed - jnp.mean(mixed, axis=-1, keepdims=True)
    spread = jnp.mean(centre * centre, axis=-1, keepdims=True)
    normed = centre * lax.rsqrt(spread + 0.00064) * head_norm_gain.reshape(heads_here, 1, 1, HEAD)
    normed = normed.transpose(1, 2, 0, 3).reshape(length_here, width_here)
    gated = (normed * jax.nn.sigmoid(gate_logits.astype(jnp.float32))).astype(jnp.bfloat16)
    sp_count = lax.axis_size("sp")
    tp_count = lax.axis_size("tp")
    capacity = max(2, 2 * TOK_DEV * TOP // (tp_count * sp_count))
    cap = -(-capacity // 16) * 16
    local_count = residual.shape[0]
    flat_routes = routes.reshape(-1)
    expert_ids = jnp.arange(sp_count, dtype=jnp.int32)
    chosen = (flat_routes[:, None] == expert_ids[None, :]).astype(jnp.int32)
    earlier = jnp.cumsum(chosen, axis=0) - chosen
    slot_index = jnp.sum(earlier * chosen, axis=1)
    target = flat_routes * cap + slot_index
    slots = jnp.arange(sp_count * cap, dtype=jnp.int32)
    placed = (target[:, None] == slots[None, :]).reshape(local_count, TOP, sp_count * cap)
    placed = placed.astype(jnp.float32)
    place = jnp.sum(placed, axis=1).astype(jnp.bfloat16).T
    combine = jnp.sum(placed * routing_weight[:, :, None], axis=1)
    return after_mixer(
        gated,
        output_weight,
        residual,
        expert_norm_gain[None, :],
        place,
        combine,
        expert_gate_weight,
        expert_up_weight,
        expert_down_weight,
        cap,
    )


def solution(mesh):
    placed = (
        P(("grp", "sp"), "tp"),
        P(("grp", "sp"), "tp"),
        P(("grp", "sp"), "tp"),
        P(("grp", "sp"), "tp"),
        P(("grp", "sp"), "tp"),
        P(("grp", "sp"), "tp"),
        P(("grp", "sp"), "tp"),
        P("tp"),
        P("tp", None),
        P(("grp", "sp", "tp"), None),
        P(),
        P(("grp", "sp", "tp"), None),
        P(("grp", "sp", "tp"), None),
        P("sp", None, "tp"),
        P("sp", None, "tp"),
        P("sp", "tp", None),
    )
    return jax.shard_map(
        body, mesh=mesh, in_specs=placed, out_specs=P(("grp", "sp", "tp"), None), check_vma=False
    )
```
